128 devices in a mesh: sp: 16 (over z, x), tp: 8 (over y, core).
Axes of the slice: x: 4, y: 4, z: 4, core: 2. Of those that a mesh axis runs over, the one named last changes fastest.
Arguments:
- a_lin: bfloat16 [16384, 1024], P('sp', 'tp'), may hold values from -6 to 6
- a_gate: bfloat16 [16384, 1024], P('sp', 'tp'), may hold values from -9 to 9
- conv_weight: bfloat16 [31, 1024], P(None, 'tp'), may hold values from -7 to 7
- ln_gain: bfloat16 [1024], P('tp'), may hold values from 0.099609375 to 1.8984375
- ln_bias: bfloat16 [1024], P('tp'), may hold values from -3 to 3
- proj_weight: bfloat16 [1024, 2048], replicated, may hold values from -0.1875 to 0.1875
- residual: bfloat16 [16384, 2048], P(('sp', 'tp')), may hold values from -6 to 6
- mix_gain: bfloat16 [2048], replicated, may hold values from 0.099609375 to 1.8984375
- ffn_gain: bfloat16 [2048], replicated, may hold values from 0.099609375 to 1.8984375
- routes: int32 [16384, 2], P(('sp', 'tp')), may hold values from 0 to 15, all different within a row; in each aligned block of 128 rows (0 to 127, 128 to 255, ...) at most 20 rows name the same one
- route_weights: float32 [16384, 2], P(('sp', 'tp')), may hold values from 0.1 to 1
- gate_weight: bfloat16 [16, 2048, 7168], P('sp', None, 'tp'), may hold values from -0.125 to 0.125
- up_weight: bfloat16 [16, 2048, 7168], P('sp', None, 'tp'), may hold values from -0.125 to 0.125
- down_weight: bfloat16 [16, 7168, 2048], P('sp', 'tp'), may hold values from -0.0625 to 0.0625
- out_gain: bfloat16 [2048], replicated, may hold values from 0.099609375 to 1.8984375
Outputs:
- layer_out: bfloat16 [16384, 2048], P(('sp', 'tp'))
The draws below stay inside these ranges and needn't reach their ends.
Inputs may be any that keep to these rules, and one draw needn't show every extreme that they name: In the rows of one device (128 aligned rows) no expert is named by more than 20 routes, a bound that some block reaches; the entries of one row differ.
All inputs are finite; a program needn't handle non-finite values.
Results may differ from the reference program's by a relative error of at most 0.018.
Values may be sent and summed in bfloat16 or wider, within the bound.
No kernel may reach another device: no remote copies, remote signals or barrier semaphores. Data moves between devices by JAX's collectives and lax.ppermute only.
A program may use at most 128 MiB of HBM per device.

```python
import math
import jax
import jax.numpy as jnp
import numpy as np
from jax import lax

D = 2048
D_A = 1024
FF = 7168
CONV = 31
TOPK = 2
TOK_DEV = 128
TOKENS = 16384
EXPERTS = 16
CAP = 20
N_SP = 16
N_TP = 8


def draw_conv_weight(key, part):
    first_key, second_key = jax.random.split(jax.random.fold_in(key, 17))
    filter_taps = jax.random.uniform(first_key, (CONV, D_A), jnp.float32, -1.0, 1.0)
    roughness = jnp.exp(jax.random.uniform(second_key, (D_A,), jnp.float32, -0.7, 0.7))
    position = jnp.arange(D_A, dtype=jnp.float32) / D_A
    rising = 3.0 ** position
    values = filter_taps * (3.0 / CONV) ** 0.5 * roughness[None, :] * rising[None, :]
    return values.astype(jnp.bfloat16)


def levels(key, dims, pieces, low, top_value):
    def one(dim, blocks):
        draws = jax.random.uniform(jax.random.fold_in(jax.random.fold_in(key, 6), dim), (blocks,), jnp.float32, low / len(pieces), top_value / len(pieces))
        return jnp.repeat(jnp.exp(draws), dims[dim] // blocks).reshape((-1,) + (1,) * (len(dims) - dim - 1))

    loudness = one(*pieces[0])
    for cut in pieces[1:]:
        loudness = loudness * one(*cut)
    return loudness


def routed_block(rng, own, number, rows, count, top, reach, skew):
    order = jax.random.permutation(rng, count)
    crowded, usual = shares(count, rows * top, reach, skew, True), shares(count, rows * top, reach, skew, False)
    places = jnp.arange(count)

    def named(lengths, offset_by):
        used = int((lengths > 0).sum())
        fixed = max(1, used // 4)
        passed = fixed + (places - fixed + offset_by * (used - fixed)) % max(1, count - fixed)
        return jnp.zeros((count,), jnp.int32).at[order[jnp.where(places < fixed, places, passed)]].set(jnp.asarray(lengths, jnp.int32))

    lengths = jnp.where(number % 4 == 0, named(crowded, number // 4), named(usual, number - number // 4 - 1))
    mixed = jax.random.permutation(jax.random.fold_in(own, 3), count)
    donor, sink = mixed[0:count // 2 * 2:2], mixed[1:count // 2 * 2:2]
    margin = jnp.minimum(lengths[donor] - 1, reach - lengths[sink]) // 2
    margin = jnp.where((donor == order[0]) | (sink == order[0]) | (lengths[sink] == 0), 0, jnp.maximum(margin, 0))
    passed = jax.random.randint(jax.random.fold_in(own, 4), (count // 2,), 0, 1 << 20) % (margin + 1)
    lengths = lengths.at[donor].add(-passed).at[sink].add(passed)
    items = jnp.searchsorted(jnp.cumsum(lengths), jnp.arange(rows * top), side="right").astype(jnp.int32)
    listing = items.reshape(top, rows).T
    listing = listing[jax.random.permutation(jax.random.fold_in(own, 1), rows)]
    offset_by = jax.random.randint(jax.random.fold_in(own, 2), (rows, 1), 0, top)
    return jnp.take_along_axis(listing, (jnp.arange(top)[None, :] + offset_by) % top, axis=1)


def shares(number_of, total, limit, skew, full):
    loads = [(1 << 20) // math.isqrt(grade ** skew) + 1 for grade in range(1, number_of + 1)]
    largest = limit if full else min(limit, max(-(-total // number_of), total * loads[0] // sum(loads)))
    least = 1 if total - largest >= number_of - 1 else 0
    counts, rest = [largest] + [least] * (number_of - 1), total - largest - least * (number_of - 1)
    while rest > 0:
        movable = [i for i in range(1, number_of) if counts[i] < largest] or [i for i in range(1, number_of) if counts[i] < limit]
        whole, remaining = sum([loads[i] for i in movable]), rest
        for i in movable:
            addition = min(limit - counts[i], max(1, remaining * loads[i] // whole), rest)
            counts[i] = counts[i] + addition
            rest = rest - addition
    return np.array(counts)


def normal_values(key, extent, deviation, bound, shards=(), kind=jnp.bfloat16):
    values = deviation * jax.random.normal(key, extent, jnp.float32)
    if shards:
        values = values * levels(key, extent, shards, -0.22, 0.18)
    return jnp.clip(values, -bound, bound).astype(kind)


def setup_inputs(seed: int = 0) -> dict:
    splits = jax.random.split(jax.random.key(seed), 16)
    a_lin = normal_values(splits[0], (TOKENS, D_A), 1.0, 6.0, ((0, 16), (1, 8)))
    a_gate = normal_values(splits[1], (TOKENS, D_A), 1.5, 9.0, ((0, 16), (1, 8)))
    conv_weight = draw_conv_weight(jax.random.fold_in(splits[15], 71), 0)
    ln_gain = jnp.clip(1.0 + 0.18 * jax.random.normal(splits[3], (D_A,), jnp.float32), 0.099609375, 1.8984375).astype(jnp.bfloat16)
    ln_bias = normal_values(splits[4], (D_A,), 0.5, 3.0, ((0, 8),))
    proj_weight = normal_values(splits[5], (D_A, D), D_A ** -0.5, 0.1875)
    residual = normal_values(splits[6], (TOKENS, D), 1.0, 6.0, ((0, 128),))
    mix_gain = jnp.clip(1.0 + 0.18 * jax.random.normal(splits[7], (D,), jnp.float32), 0.099609375, 1.8984375).astype(jnp.bfloat16)
    ffn_gain = jnp.clip(1.0 + 0.18 * jax.random.normal(splits[8], (D,), jnp.float32), 0.099609375, 1.8984375).astype(jnp.bfloat16)
    routes_keys = jax.random.split(jax.random.fold_in(splits[9], 1), TOKENS // TOK_DEV)
    routes_turns = jax.random.permutation(jax.random.fold_in(splits[9], 3), TOKENS // TOK_DEV)
    routes = jax.vmap(lambda own, number: routed_block(jax.random.fold_in(splits[9], 2), own, number, TOK_DEV, EXPERTS, TOPK, CAP, 2))(routes_keys, routes_turns).reshape((TOKENS, TOPK))
    route_weights = jnp.clip(0.1 + 0.9 * jax.random.uniform(splits[10], (TOKENS, TOPK), jnp.float32) ** levels(splits[10], (TOKENS, TOPK), ((0, 128),), -0.2, 0.2), 0.1, 1.0)
    gate_weight = normal_values(splits[11], (EXPERTS, D, FF), D ** -0.5, 0.125, ((0, 16), (2, 8)))
    up_weight = normal_values(splits[12], (EXPERTS, D, FF), D ** -0.5, 0.125, ((0, 16), (2, 8)))
    down_weight = normal_values(splits[13], (EXPERTS, FF, D), FF ** -0.5, 0.0625, ((0, 16), (1, 8)))
    out_gain = jnp.clip(1.0 + 0.18 * jax.random.normal(splits[14], (D,), jnp.float32), 0.099609375, 1.8984375).astype(jnp.bfloat16)
    return dict(a_lin=a_lin, a_gate=a_gate, conv_weight=conv_weight, ln_gain=ln_gain, ln_bias=ln_bias, proj_weight=proj_weight, residual=residual, mix_gain=mix_gain, ffn_gain=ffn_gain, routes=routes, route_weights=route_weights, gate_weight=gate_weight, up_weight=up_weight, down_weight=down_weight, out_gain=out_gain)


def reference(a_lin, a_gate, conv_weight, ln_gain, ln_bias, proj_weight, residual, mix_gain, ffn_gain, routes, route_weights, gate_weight, up_weight, down_weight, out_gain):
    gated = (a_lin.astype(jnp.float32) * jax.nn.sigmoid(a_gate.astype(jnp.float32))).astype(jnp.bfloat16)
    padded = jnp.concatenate([jnp.zeros((CONV - 1, D_A), jnp.bfloat16), gated], 0).astype(jnp.float32)
    filter_taps = conv_weight.astype(jnp.float32)
    conv_out = filter_taps[0] * padded[0:TOKENS]
    for offset in range(1, CONV):
        conv_out = conv_out + filter_taps[offset] * padded[offset:offset + TOKENS]
    row_total = lax.optimization_barrier(jnp.sum(conv_out, axis=1))
    squares = lax.optimization_barrier(jnp.sum(conv_out * conv_out, axis=1))
    row_mean = row_total / D_A
    row_var = squares / D_A - row_mean * row_mean
    scaled = (conv_out - row_mean[:, None]) * lax.rsqrt(row_var[:, None] + 1e-05)
    scaled = scaled * ln_gain.astype(jnp.float32) + ln_bias.astype(jnp.float32)
    activated = jax.nn.silu(scaled).astype(jnp.bfloat16)
    branch = jnp.dot(activated, proj_weight, preferred_element_type=jnp.float32).astype(jnp.bfloat16)
    branch_f = lax.optimization_barrier(branch).astype(jnp.float32)
    branch_scale = lax.rsqrt(lax.optimization_barrier(jnp.mean(branch_f * branch_f, axis=1, keepdims=True)) + 1e-06)
    stream = residual.astype(jnp.float32) + branch_f * branch_scale * mix_gain.astype(jnp.float32)
    stream_scale = lax.rsqrt(lax.optimization_barrier(jnp.mean(stream * stream, axis=1, keepdims=True)) + 1e-06)
    normed = (stream * stream_scale * ffn_gain.astype(jnp.float32)).astype(jnp.bfloat16)
    blocks = N_SP * N_TP
    flat_routes = routes.reshape(blocks, TOK_DEV * TOPK)
    matches = (flat_routes[:, :, None] == jnp.arange(EXPERTS, dtype=jnp.int32)[None, None, :]).astype(jnp.int32)
    before = jnp.cumsum(matches, axis=1) - matches
    slot_index = lax.optimization_barrier(jnp.sum(before * matches, axis=2))
    block_ids = jnp.arange(blocks, dtype=jnp.int32)[:, None]
    target = ((flat_routes * blocks + block_ids) * CAP + slot_index).reshape(-1).astype(jnp.int32)
    source_rows = jnp.repeat(normed, TOPK, axis=0)
    buffer = jnp.zeros((EXPERTS * blocks * CAP, D), jnp.bfloat16).at[target].set(source_rows)
    buffer = buffer.reshape(EXPERTS, blocks * CAP, D)
    width_block = FF // N_TP

    def one_expert(inputs):
        rows_in, w_gate, w_up, w_down = inputs
        accum = jnp.zeros((rows_in.shape[0], D), jnp.float32)
        for part_index in range(N_TP):
            low = part_index * width_block
            gate_proj = jnp.dot(rows_in, w_gate[:, low:low + width_block], preferred_element_type=jnp.float32)
            up_proj = jnp.dot(rows_in, w_up[:, low:low + width_block], preferred_element_type=jnp.float32)
            hidden = (jax.nn.silu(gate_proj) * up_proj).astype(jnp.bfloat16)
            partial_out = jnp.dot(hidden, w_down[low:low + width_block], preferred_element_type=jnp.float32).astype(jnp.bfloat16)
            accum = accum + lax.optimization_barrier(partial_out).astype(jnp.float32)
        return accum.astype(jnp.bfloat16)
    results = lax.map(one_expert, (buffer, gate_weight, up_weight, down_weight))
    results = lax.optimization_barrier(results).reshape(EXPERTS * blocks * CAP, D)
    picked = results[target].astype(jnp.float32).reshape(TOKENS, TOPK, D)
    expert_mix = lax.optimization_barrier(jnp.sum(picked * route_weights[:, :, None], axis=1))
    mix_scale = lax.rsqrt(lax.optimization_barrier(jnp.mean(expert_mix * expert_mix, axis=1, keepdims=True)) + 1e-06)
    return (stream + expert_mix * mix_scale * out_gain.astype(jnp.float32)).astype(jnp.bfloat16)
```

```python
import jax
import jax.numpy as jnp
from jax import lax
from jax.experimental import pallas as pl
from jax.experimental.pallas import tpu as pltpu
from jax.sharding import PartitionSpec as P

D = 2048
D_A = 1024
CONV = 31
HALO = 32
CAP = 20
PAD = 24
EXPERTS = 16
TOK = 128
F32 = jnp.float32
BF16 = jnp.bfloat16
EXPERT_FLOPS = 2 * 2 * 3 * D * 896


def dot(a, b):
    return jnp.dot(a, b, preferred_element_type=F32)


def pack_kernel(a_lin, a_gate, taps, gain, bias, packed):
    gated = (a_lin[...].astype(F32) * jax.nn.sigmoid(a_gate[...].astype(F32))).astype(BF16)
    blank = jnp.zeros((16, 128), BF16)
    for t in range(8):
        if t == 0:
            packed[t, HALO : HALO + TOK] = gated[:TOK]
        else:
            packed[t, : HALO + TOK] = gated[TOK * t - HALO : TOK * (t + 1)]
        packed[t, HALO + TOK : HALO + TOK + CONV] = taps[...]
        packed[t, HALO + TOK + CONV : HALO + TOK + 32] = blank[:1]
        packed[t, HALO + TOK + 32 :] = blank
        packed[t, HALO + TOK + 32 : HALO + TOK + 33] = gain[...]
        packed[t, HALO + TOK + 33 : HALO + TOK + 34] = bias[...]


def pack(a_lin, a_gate, taps, gain, bias):
    return pl.pallas_call(
        pack_kernel,
        out_shape=jax.ShapeDtypeStruct((8, HALO + TOK + 48, 128), BF16),
        compiler_params=pltpu.CompilerParams(vmem_limit_bytes=16 * 2**20),
        name="pack",
    )(a_lin, a_gate, taps, gain[None], bias[None])


def front_kernel(
    got, proj, residual, mix_gain, ffn_gain, routes, slots, outgoing, stream_out, hits_out, rows_f, conv, proj_v, sem
):
    load = pltpu.make_async_copy(proj, proj_v, sem)
    load.start()
    total = jnp.zeros((TOK, 128), F32)
    squares = jnp.zeros((TOK, 128), F32)
    for j in range(8):
        rows_f[...] = got[j].astype(F32)
        acc = rows_f[HALO + TOK : HALO + TOK + 1, :] * rows_f[2 : 2 + TOK, :]
        for k in range(1, CONV):
            tap = rows_f[HALO + TOK + k : HALO + TOK + k + 1, :]
            acc = acc + tap * rows_f[2 + k : 2 + k + TOK, :]
        total = total + acc
        squares = squares + acc * acc
        conv[:, 128 * j : 128 * (j + 1)] = acc
    mean = jnp.sum(total, axis=1, keepdims=True) / D_A
    var = jnp.sum(squares, axis=1, keepdims=True) / D_A - mean * mean
    inv = lax.rsqrt(var + 1e-05)
    acts = []
    for j in range(8):
        gain = got[j, HALO + TOK + 32 : HALO + TOK + 48, :].astype(F32)
        scaled = (conv[:, 128 * j : 128 * (j + 1)] - mean) * inv
        scaled = scaled * gain[0:1] + gain[1:2]
        acts.append(jax.nn.silu(scaled).astype(BF16))
    load.wait()
    branch = dot(jnp.concatenate(acts, axis=1), proj_v[...])
    branch = branch.astype(BF16).astype(F32)
    scale = lax.rsqrt(jnp.mean(branch * branch, axis=1, keepdims=True) + 1e-06)
    stream = residual[...].astype(F32) + branch * scale * mix_gain[...].astype(F32)
    stream_out[...] = stream
    scale = lax.rsqrt(jnp.mean(stream * stream, axis=1, keepdims=True) + 1e-06)
    normed = (stream * scale * ffn_gain[...].astype(F32)).astype(BF16)
    expert, slot = slots[0:1], slots[1:2]
    named = (routes[:, 0:1] == expert) | (routes[:, 1:2] == expert)
    earlier = lax.broadcasted_iota(jnp.int32, (TOK, TOK), 1) < lax.broadcasted_iota(
        jnp.int32, (TOK, TOK), 0
    )
    before = dot(earlier.astype(F32).astype(BF16), named.astype(F32).astype(BF16))
    hits = (named & (before == slot.astype(F32))).astype(F32).astype(BF16)
    hits_out[...] = hits
    picked = lax.dot_general(
        hits, normed, (((0,), (0,)), ((), ())), preferred_element_type=F32
    ).astype(BF16)
    for e in range(EXPERTS):
        outgoing[e] = picked[PAD * e : PAD * e + CAP]


def front(got, proj, residual, mix_gain, ffn_gain, routes, slots):
    return pl.pallas_call(
        front_kernel,
        out_shape=(
            jax.ShapeDtypeStruct((EXPERTS, CAP, D), BF16),
            jax.ShapeDtypeStruct((TOK, D), F32),
            jax.ShapeDtypeStruct((TOK, EXPERTS * PAD), BF16),
        ),
        scratch_shapes=[
            pltpu.VMEM((got.shape[1], 128), F32),
            pltpu.VMEM((TOK, D_A), F32),
            pltpu.VMEM((D_A, D), BF16),
            pltpu.SemaphoreType.DMA,
        ],
        in_specs=[
            pl.BlockSpec(memory_space=pltpu.VMEM if i != 1 else pltpu.HBM) for i in range(7)
        ],
        compiler_params=pltpu.CompilerParams(vmem_limit_bytes=24 * 2**20),
        name="front",
    )(got, proj, residual, mix_gain[None], ffn_gain[None], routes, slots)


def tail_kernel(returned, hits, routes, weights, slots, stream, out_gain, out, rows):
    for e in range(EXPERTS):
        rows[PAD * e : PAD * e + CAP] = returned[e]
        rows[PAD * e + CAP : PAD * (e + 1)] = jnp.zeros((PAD - CAP, D), BF16)
    mix = jnp.zeros((TOK, D), F32)
    for k in range(2):
        chosen = jnp.where(routes[:, k : k + 1] == slots[0:1], hits[...].astype(F32), 0.0)
        mix = mix + weights[:, k : k + 1] * dot(chosen.astype(BF16), rows[...])
    scale = lax.rsqrt(jnp.mean(mix * mix, axis=1, keepdims=True) + 1e-06)
    out[...] = (stream[...] + mix * scale * out_gain[...].astype(F32)).astype(BF16)


def tail(returned, hits, routes, weights, slots, stream, out_gain):
    return pl.pallas_call(
        tail_kernel,
        out_shape=jax.ShapeDtypeStruct((TOK, D), BF16),
        scratch_shapes=[pltpu.VMEM((EXPERTS * PAD, D), BF16)],
        compiler_params=pltpu.CompilerParams(vmem_limit_bytes=24 * 2**20),
        name="tail",
    )(returned, hits, routes, weights, slots, stream, out_gain[None])


def expert_kernel(mine, others, w_gate, w_up, w_down, mine_out, others_out):
    for rows, out in ((mine, mine_out), (others, others_out)):
        value = rows[...]
        gate = dot(value, w_gate[0])
        up = dot(value, w_up[0])
        hidden = (jax.nn.silu(gate) * up).astype(BF16)
        out[...] = dot(hidden, w_down[0]).astype(BF16)


def expert(mine, others, w_gate, w_up, w_down):
    count = mine.shape[0]
    made = jax.ShapeDtypeStruct((count, D), BF16)
    return pl.pallas_call(
        expert_kernel,
        out_shape=(made, made),
        cost_estimate=pl.CostEstimate(
            flops=EXPERT_FLOPS * count, transcendentals=0, bytes_accessed=8 * count * D
        ),
        compiler_params=pltpu.CompilerParams(vmem_limit_bytes=36 * 2**20),
        name="expert",
    )(mine, others, w_gate, w_up, w_down)


def forward(value):
    return lax.ppermute(value, "tp", [(t, (t + (-2 if t % 2 else 2)) % 8) for t in range(8)])


def backward(value):
    return lax.ppermute(value, "tp", [(t, (t + (2 if t % 2 else -2)) % 8) for t in range(8)])


def sibling(value):
    return lax.ppermute(value, "tp", [(t, t ^ 1) for t in range(8)])


def plus(*terms):
    total = terms[0].astype(F32)
    for term in terms[1:]:
        total = total + term.astype(F32)
    return total.astype(BF16)


def per_device(
    a_lin,
    a_gate,
    conv_weight,
    ln_gain,
    ln_bias,
    proj_weight,
    residual,
    mix_gain,
    ffn_gain,
    routes,
    route_weights,
    gate_weight,
    up_weight,
    down_weight,
    out_gain,
):
    last = a_lin.shape[0] - HALO
    edge = a_lin[last:].astype(F32) * jax.nn.sigmoid(a_gate[last:].astype(F32))
    edge = lax.ppermute(edge.astype(BF16), "sp", [(s, s + 1) for s in range(15)])
    packed = pack(a_lin, a_gate, conv_weight, ln_gain, ln_bias)
    packed = packed.at[0, :HALO].set(edge)
    got = lax.all_to_all(packed, "tp", split_axis=0, concat_axis=0, tiled=True)
    column = jnp.arange(EXPERTS * PAD, dtype=jnp.int32)
    slots = jnp.stack([column // PAD, column % PAD])
    outgoing, stream, hits = front(got, proj_weight, residual, mix_gain, ffn_gain, routes, slots)

    weights = (gate_weight, up_weight, down_weight)
    arrived = lax.all_to_all(outgoing, "sp", split_axis=0, concat_axis=0, tiled=True)
    own = arrived.reshape(EXPERTS * CAP, D)
    near_m = forward(own)
    own_o = sibling(own)
    near_o = forward(own_o)
    far_m = forward(near_m)
    via_m = sibling(near_m)
    p_own_m, p_own_o = expert(own, own_o, *weights)
    near_m, via_m, p_own_m, p_own_o = lax.optimization_barrier((near_m, via_m, p_own_m, p_own_o))
    p_near_m, p_via_m = expert(near_m, via_m, *weights)
    far_o = sibling(far_m)
    via_o = sibling(near_o)
    near_o, via_o, p_near_m, p_via_m = lax.optimization_barrier((near_o, via_o, p_near_m, p_via_m))
    p_near_o, p_via_o = expert(near_o, via_o, *weights)
    far_m, far_o, p_near_o, p_via_o = lax.optimization_barrier((far_m, far_o, p_near_o, p_via_o))
    p_far_m, p_far_o = expert(far_m, far_o, *weights)
    r_near_o = backward(plus(p_near_o, sibling(p_via_o)))
    r_far = backward(plus(p_far_m, sibling(p_far_o)))
    r_near_m = backward(plus(p_near_m, sibling(p_via_m), r_far))
    summed = plus(p_own_m, r_near_m, sibling(plus(p_own_o, r_near_o)))
    back = summed.reshape(EXPERTS, CAP, D)
    returned = lax.all_to_all(back, "sp", split_axis=0, concat_axis=0, tiled=True)
    return tail(
        returned, hits, routes, route_weights, slots, stream, out_gain
    )


def solution(mesh):
    return jax.shard_map(
        per_device,
        mesh=mesh,
        in_specs=(
            P("sp", "tp"),
            P("sp", "tp"),
            P(None, "tp"),
            P("tp"),
            P("tp"),
            P(),
            P(("sp", "tp"), None),
            P(),
            P(),
            P(("sp", "tp"), None),
            P(("sp", "tp"), None),
            P("sp", None, "tp"),
            P("sp", None, "tp"),
            P("sp", "tp", None),
            P(),
        ),
        out_specs=P(("sp", "tp"), None),
        check_vma=False,
    )
```
